32 devices in a mesh: sp: 16 (over z, y, x), tp: 2 (over core).
Axes of the slice: x: 2, y: 2, z: 4, core: 2. Of those that a mesh axis runs over, the one named last changes fastest.
Arguments:
- residual: bfloat16 [6144, 2048], P('sp'), may hold values from -6 to 6
- queries: bfloat16 [6144, 2048], P('sp', 'tp'), may hold values from -48 to 48
- keys: bfloat16 [6144, 2048], P('sp', 'tp'), may hold values from -48 to 48
- values: bfloat16 [6144, 2048], P('sp', 'tp'), may hold values from -6 to 6
- gate_cache: float32 [6144, 32], P('sp', 'tp'), may hold values from -1544 to 0, as said below
- doc_ids: int32 [6144], P('sp'), may hold values from 0 to 7, never falling along the last dimension, each value on 1 to 1536 neighbouring positions
- out_weight: bfloat16 [2048, 2048], P('tp'), may hold values from -1 to 1
- mix_gain: float32 [2048], replicated, may hold values from 0.1 to 1.9
- gate_weight: bfloat16 [2048, 5120], P('sp', 'tp'), may hold values from -0.125 to 0.125
- up_weight: bfloat16 [2048, 5120], P('sp', 'tp'), may hold values from -0.125 to 0.125
- down_weight: bfloat16 [5120, 2048], P('tp', 'sp'), may hold values from -0.15625 to 0.15625
Outputs:
- layer_out: bfloat16 [6144, 2048], P(('sp', 'tp'))
The draws below stay inside these ranges and needn't reach their ends.
Inputs may be any that keep to these rules, and one draw needn't show every extreme that they name: `doc_ids`: positions of one document are consecutive; each document has 1 to 1536 positions, and one has exactly that many. `gate_cache`: no column rises from one position to the next.
All inputs are finite; a program needn't handle non-finite values.
Results may differ from the reference program's by a relative error of at most 0.018.
Values may be sent and summed in bfloat16 or wider, within the bound.
No kernel may reach another device: no remote copies, remote signals or barrier semaphores. Data moves between devices by JAX's collectives and lax.ppermute only.
A program may use at most 128 MiB of HBM per device.

```python
import math
import jax
import jax.numpy as jnp
import numpy as np
from jax import lax

D = 2048
HEAD_COUNT = 32
HEAD_DIM = 64
FF = 5120
REACH = 4
TOK_DEV = 384
TOKEN_COUNT = 6144
DOCS = 8
N_TP = 2


def drawn(key):
    base_key = jax.random.fold_in(key, 11)
    key_q, key_k = jax.random.split(base_key, 2)
    col_count = HEAD_COUNT * HEAD_DIM
    queries = jax.random.normal(key_q, (TOKEN_COUNT, col_count), jnp.float32)
    keys = jax.random.normal(key_k, (TOKEN_COUNT, col_count), jnp.float32)
    return (jnp.clip(queries, -48.0, 48.0), jnp.clip(keys, -48.0, 48.0))


def draw_queries(key, part):
    return drawn(key)[0].astype(jnp.bfloat16)


def draw_keys(key, part):
    return drawn(key)[1].astype(jnp.bfloat16)


def draw_gate_cache(key, part):
    base_key = jax.random.fold_in(key, 23)
    key_h, key_r, key_s, key_b, key_u, key_position, key_document = jax.random.split(base_key, 7)
    head_order = jax.random.permutation(key_h, HEAD_COUNT)
    slow_heads = head_order < HEAD_COUNT // 2
    fast_rate = jnp.exp(jax.random.uniform(key_r, (HEAD_COUNT,), jnp.float32, math.log(1.0 / 100.0), math.log(1.0 / 30.0)))
    slow_rate = jax.random.uniform(key_s, (HEAD_COUNT,), jnp.float32, 0.5, 2.0) / TOKEN_COUNT
    head_rate = jnp.where(slow_heads, slow_rate, fast_rate)
    blocks = TOKEN_COUNT // TOK_DEV
    factor = jnp.exp(jax.random.uniform(key_b, (blocks,), jnp.float32, math.log(0.4), math.log(2.5)))
    factor_rows = jnp.repeat(factor, TOK_DEV)
    wobble = jax.random.uniform(key_u, (TOKEN_COUNT, HEAD_COUNT), jnp.float32, 0.2, 1.8)
    logarithm_gate = -head_rate[None, :] * factor_rows[:, None] * wobble
    spike_start = jax.random.randint(key_position, (8,), 0, TOKEN_COUNT)
    spike_length = jnp.log(jax.random.uniform(key_document, (8, HEAD_COUNT), jnp.float32, 0.5, 0.8))
    logarithm_gate = logarithm_gate.at[spike_start].add(spike_length)
    return jnp.cumsum(logarithm_gate, axis=0)


def block_scale(stream_key, shape, cuts, least, largest):
    def one(position, parts):
        heights = jax.random.uniform(jax.random.fold_in(jax.random.fold_in(stream_key, 6), position), (parts,), jnp.float32, least / len(cuts), largest / len(cuts))
        return jnp.repeat(jnp.exp(heights), shape[position] // parts).reshape((-1,) + (1,) * (len(shape) - position - 1))

    loudness = one(*cuts[0])
    for cut in cuts[1:]:
        loudness = loudness * one(*cut)
    return loudness


def length_profile(amount, total, limit, slope):
    portions = [(1 << 20) // math.isqrt(rank ** slope) + 1 for rank in range(2, amount + 1)]
    surplus, given = total - limit - (amount - 1), [1] * (amount - 1)
    while surplus > 0:
        candidates = [i for i in range(amount - 1) if given[i] < limit]
        whole, remaining = sum([portions[i] for i in candidates]), surplus
        for i in candidates:
            addition = min(limit - given[i], max(1, remaining * portions[i] // whole), surplus)
            given[i] = given[i] + addition
            surplus = surplus - addition
    return np.array([limit] + given)


def ragged_sizes(rng, count, total, most, slope):
    if count == 2:
        one = jax.random.randint(rng, (), max(1, total - most), min(most, total - 1) + 1)
        return jnp.stack([one, total - one])
    tallies = jnp.asarray(length_profile(count, total, most, slope), jnp.int32)
    twos = (count - 1) // 2
    source_of, taker = tallies[1:1 + 2 * twos:2], tallies[2:2 + 2 * twos:2]
    margin = jnp.minimum(source_of - 1, most - taker)
    shifted = jax.random.randint(jax.random.fold_in(rng, 1), (twos,), 0, 1 << 20) % (margin + 1)
    tallies = tallies.at[1:1 + 2 * twos:2].set(source_of - shifted).at[2:2 + 2 * twos:2].set(taker + shifted)
    return tallies[jax.random.permutation(jax.random.fold_in(rng, 2), count)]


def noise(rng, dims, scale, reach, pieces=(), held_as=jnp.bfloat16):
    level = block_scale(rng, dims, pieces, -0.22, 0.18) if pieces else 1.0
    drawn = jax.random.normal(rng, dims, jnp.float32) * scale * level
    return jnp.minimum(jnp.maximum(drawn, -reach), reach).astype(held_as)


def setup_inputs(seed: int = 0) -> dict:
    streams_of = jax.random.split(jax.random.key(seed), 12)
    return {
        "residual": noise(streams_of[0], (TOKEN_COUNT, D), 1.0, 6.0, ((0, 16),)),
        "queries": draw_queries(jax.random.fold_in(streams_of[11], 71), 0),
        "keys": draw_keys(jax.random.fold_in(streams_of[11], 71), 0),
        "values": noise(streams_of[3], (TOKEN_COUNT, HEAD_COUNT * HEAD_DIM), 1.0, 6.0, ((0, 16), (1, 2))),
        "gate_cache": draw_gate_cache(jax.random.fold_in(streams_of[11], 71), 0),
        "doc_ids": jnp.searchsorted(jnp.cumsum(ragged_sizes(streams_of[5], DOCS, TOKEN_COUNT, REACH * TOK_DEV, 0)), jnp.arange(TOKEN_COUNT), side="right").astype(jnp.int32),
        "out_weight": noise(streams_of[6], (HEAD_COUNT * HEAD_DIM, D), (HEAD_COUNT * HEAD_DIM // 64) ** -0.5, 1.0, ((0, 2),)),
        "mix_gain": jnp.clip(1.0 + 0.18 * jax.random.normal(streams_of[7], (D,), jnp.float32), 0.1, 1.9),
        "gate_weight": noise(streams_of[8], (D, FF), D ** -0.5, 0.125, ((0, 16), (1, 2))),
        "up_weight": noise(streams_of[9], (D, FF), D ** -0.5, 0.125, ((0, 16), (1, 2))),
        "down_weight": noise(streams_of[10], (FF, D), (FF // 4) ** -0.5, 0.15625, ((0, 2), (1, 16))),
    }


EPSILON = 1e-06
NEGATIVE = -1e+30

def group_sum(activations, weight, groups):
    row_count = activations.shape[0]
    inner_cols = activations.shape[1] // groups
    left_grouped = activations.reshape(row_count, groups, inner_cols).transpose(1, 0, 2)
    right_grouped = weight.reshape(groups, inner_cols, weight.shape[1])

    def add_group(running, operands):
        partial_value = jnp.dot(operands[0], operands[1], preferred_element_type=jnp.float32)
        rounded = lax.optimization_barrier(partial_value.astype(jnp.bfloat16))
        return (running + rounded.astype(jnp.float32), None)
    zeros_init = jnp.zeros((row_count, weight.shape[1]), jnp.float32)
    running, ignored = lax.scan(add_group, zeros_init, (left_grouped, right_grouped))
    return running

def normalize(middle, gain):
    widened = middle.astype(jnp.float32)
    factor = lax.rsqrt(lax.optimization_barrier(jnp.mean(widened * widened, axis=-1, keepdims=True)) + EPSILON)
    return (widened * factor * gain).astype(jnp.bfloat16)

def attend(queries, keys, values, gate_cache, doc_ids):
    tokens = queries.shape[0]
    doc_span = REACH * TOK_DEV
    block_rows = math.gcd(tokens, 512)
    key_count = doc_span + block_rows
    head_shape = (tokens, HEAD_COUNT, HEAD_DIM)
    query_heads = queries.reshape(head_shape)
    pad_rows = ((doc_span, 0), (0, 0), (0, 0))
    key_heads = jnp.pad(keys.reshape(head_shape), pad_rows)
    value_heads = jnp.pad(values.reshape(head_shape), pad_rows)
    cache_pad = jnp.pad(gate_cache, ((doc_span, 0), (0, 0)))
    docs_pad = jnp.pad(doc_ids, (doc_span, 0), constant_values=-1)
    score_scale = HEAD_DIM ** (-0.5)

    def one_block(block_index):
        start_row = (block_index * block_rows).astype(jnp.int32)
        query_block = lax.dynamic_slice_in_dim(query_heads, start_row, block_rows, 0).astype(jnp.float32)
        key_block = lax.dynamic_slice_in_dim(key_heads, start_row, key_count, 0).astype(jnp.float32)
        value_block = lax.dynamic_slice_in_dim(value_heads, start_row, key_count, 0).astype(jnp.float32)
        query_cache = lax.dynamic_slice_in_dim(gate_cache, start_row, block_rows, 0)
        key_cache = lax.dynamic_slice_in_dim(cache_pad, start_row, key_count, 0)
        query_docs = lax.dynamic_slice_in_dim(doc_ids, start_row, block_rows, 0)
        key_docs = lax.dynamic_slice_in_dim(docs_pad, start_row, key_count, 0)
        query_pos = start_row + jnp.arange(block_rows, dtype=jnp.int32)
        key_pos = start_row - doc_span + jnp.arange(key_count, dtype=jnp.int32)
        visible = (key_pos[None, :] <= query_pos[:, None]) & (key_pos[None, :] >= 0) & (key_docs[None, :] == query_docs[:, None])
        scores = jnp.einsum('qhd,khd->hqk', query_block, key_block) * score_scale
        scores = scores + query_cache.T[:, :, None] - key_cache.T[:, None, :]
        scores = jnp.where(visible[None], scores, NEGATIVE)
        row_max = lax.optimization_barrier(jnp.max(scores, axis=-1, keepdims=True))
        exp_scores = jnp.exp(scores - row_max)
        weights = (exp_scores / lax.optimization_barrier(jnp.sum(exp_scores, axis=-1, keepdims=True))).astype(jnp.bfloat16)
        weights = lax.optimization_barrier(weights)
        mixed_out = jnp.einsum('hqk,khd->qhd', weights.astype(jnp.float32), value_block)
        return mixed_out.astype(jnp.bfloat16)
    blocks = lax.map(one_block, jnp.arange(tokens // block_rows, dtype=jnp.int32))
    return blocks.reshape(tokens, HEAD_COUNT * HEAD_DIM)

def reference(residual, queries, keys, values, gate_cache, doc_ids, out_weight, mix_gain, gate_weight, up_weight, down_weight):
    attended = attend(queries, keys, values, gate_cache, doc_ids)
    projected = group_sum(attended, out_weight, N_TP)
    middle = (residual.astype(jnp.float32) + projected).astype(jnp.bfloat16)
    normed = normalize(middle, mix_gain)
    gate_proj = jnp.dot(normed, gate_weight, preferred_element_type=jnp.float32)
    up_proj = jnp.dot(normed, up_weight, preferred_element_type=jnp.float32)
    hidden = (jax.nn.silu(gate_proj) * up_proj).astype(jnp.bfloat16)
    lowered = group_sum(hidden, down_weight, N_TP)
    return (middle.astype(jnp.float32) + lowered).astype(jnp.bfloat16)
```

```python
import functools
import math

import jax
import jax.numpy as jnp
from jax import lax
from jax.experimental import pallas as pl
from jax.experimental.pallas import tpu as pltpu
from jax.sharding import PartitionSpec as P

REACH = 4

EPSILON = 1e-06
NEGATIVE = -1e30


def normalize(middle, gain):
    widened = middle.astype(jnp.float32)
    factor = lax.rsqrt(jnp.mean(widened * widened, axis=-1, keepdims=True) + EPSILON)
    return (widened * factor * gain).astype(jnp.bfloat16)


def attend_kernel(low_ref, q_ref, qdoc_ref, kv_ref, aux_ref, out_ref, acc_ref, *, heads, block, scale):
    width = q_ref.shape[1]
    head_size = width // heads
    step = pl.program_id(0)
    diagonal = (kv_ref.shape[0] // block) // 2 + step
    lane = lax.broadcasted_iota(jnp.int32, (1, width), 1) // head_size
    q = q_ref[...] * jnp.asarray(scale, q_ref.dtype)
    q_parts = [jnp.where(lane == h, q, jnp.zeros_like(q)) for h in range(heads)]
    qdoc = qdoc_ref[...]
    acc_ref[...] = jnp.zeros_like(acc_ref)

    def chunk(index, carry, causal):
        start = pl.multiple_of(index * block, block)
        k = kv_ref[pl.ds(start, block), :width]
        v = kv_ref[pl.ds(start, block), width:]
        aux = aux_ref[:, pl.ds(start, block)]
        seen = aux[heads : heads + 1] == qdoc
        if causal:
            row = lax.broadcasted_iota(jnp.int32, (block, block), 0)
            col = lax.broadcasted_iota(jnp.int32, (block, block), 1)
            seen = seen & (col <= row)
        new = []
        decay = jnp.zeros((block, width), jnp.float32)
        added = jnp.zeros((block, width), jnp.float32)
        for h in range(heads):
            top, total = carry[h]
            scores = lax.dot_general(
                q_parts[h], k, (((1,), (1,)), ((), ())), preferred_element_type=jnp.float32
            )
            scores = jnp.where(seen, scores - aux[h : h + 1], NEGATIVE)
            new_top = jnp.maximum(top, jnp.max(scores, axis=-1, keepdims=True))
            weights = jnp.exp(scores - new_top)
            shrink = jnp.exp(top - new_top)
            total = total * shrink + jnp.sum(weights, axis=-1, keepdims=True)
            v_part = jnp.where(lane == h, v, jnp.zeros_like(v))
            added = added + jnp.dot(
                weights.astype(v.dtype), v_part, preferred_element_type=jnp.float32
            )
            decay = jnp.where(lane == h, shrink, decay)
            new.append((new_top, total))
        acc_ref[...] = acc_ref[...] * decay + added
        return tuple(new)

    first = tuple(
        (jnp.full((block, 1), NEGATIVE, jnp.float32), jnp.zeros((block, 1), jnp.float32))
        for h in range(heads)
    )
    carry = lax.fori_loop(
        low_ref[step], diagonal, functools.partial(chunk, causal=False), first
    )
    carry = chunk(diagonal, carry, True)
    divisor = jnp.ones((block, width), jnp.float32)
    for h in range(heads):
        divisor = jnp.where(lane == h, carry[h][1], divisor)
    out_ref[...] = (acc_ref[...] / divisor).astype(out_ref.dtype)


def attend(q, kv, aux, docs, heads, scale):
    rows, width = q.shape
    block = math.gcd(rows, 256)
    steps = rows // block
    firsts = docs[rows::block]
    low = jnp.sum((docs[None, :] < firsts[:, None]).astype(jnp.int32), axis=1) // block
    low = jnp.maximum(low, jnp.arange(steps, dtype=jnp.int32))
    keys = kv.shape[0]
    return pl.pallas_call(
        functools.partial(attend_kernel, heads=heads, block=block, scale=scale),
        grid_spec=pltpu.PrefetchScalarGridSpec(
            num_scalar_prefetch=1,
            grid=(steps,),
            in_specs=[
                pl.BlockSpec((block, width), lambda i, low: (i, 0)),
                pl.BlockSpec((block, 1), lambda i, low: (i, 0)),
                pl.BlockSpec((keys, 2 * width), lambda i, low: (0, 0)),
                pl.BlockSpec((aux.shape[0], keys), lambda i, low: (0, 0)),
            ],
            out_specs=pl.BlockSpec((block, width), lambda i, low: (i, 0)),
            scratch_shapes=[pltpu.VMEM((block, width), jnp.float32)],
        ),
        out_shape=jax.ShapeDtypeStruct((rows, width), jnp.bfloat16),
        cost_estimate=pl.CostEstimate(
            flops=4 * rows * rows * width * heads,
            bytes_accessed=2 * (rows + keys) * width * 2,
            transcendentals=rows * rows * heads,
        ),
        name="attend",
    )(low, q, docs[rows:, None], kv, aux)


def local(
    residual,
    queries,
    keys,
    values,
    gate_cache,
    doc_ids,
    out_weight,
    mix_gain,
    gate_weight,
    up_weight,
    down_weight,
):
    n_sp, n_tp = lax.axis_size("sp"), lax.axis_size("tp")
    group = REACH
    levels = n_sp // group
    sp_index, tp_index = lax.axis_index("sp"), lax.axis_index("tp")
    level, member = sp_index // group, sp_index % group
    rows, width = queries.shape
    heads_here = gate_cache.shape[1]
    head_size = width // heads_here
    heads = heads_here // group
    share = width // group
    span = rows * group

    def swap(value, mask):
        return lax.ppermute(value, "sp", [(s, s ^ mask) for s in range(n_sp)]) if mask else value

    def next_level(value):
        return lax.ppermute(value, "sp", [(s, s + group) for s in range(n_sp - group)])

    def around(value, steps):
        return lax.ppermute(
            value, "sp", [(s, (s + steps * group) % n_sp) for s in range(n_sp)]
        )

    def turn(value, steps):
        return lax.ppermute(
            value, "tp", [(t, (t + steps) % n_tp) for t in range(n_tp)]
        )

    def piece(value, index, size, axis):
        return lax.dynamic_slice_in_dim(value, index * size, size, axis)

    def put(whole, part, index, axis):
        return lax.dynamic_update_slice_in_dim(whole, part, index * part.shape[axis], axis)

    marks = jnp.concatenate([gate_cache.T, doc_ids.astype(jnp.float32)[None]], axis=0)
    kv_all = jnp.zeros((2 * span, 2 * share), keys.dtype)
    q_all = jnp.zeros((span, share), queries.dtype)
    marks_all = jnp.zeros((heads_here + 1, 2 * span), jnp.float32)
    kv_got, q_got, marks_got = [], [], []
    for mask in range(group):
        other = member ^ mask
        kv_got.append(
            swap(
                jnp.concatenate(
                    [piece(keys, other, share, 1), piece(values, other, share, 1)], axis=1
                ),
                mask,
            )
        )
        marks_got.append(swap(marks, mask))
    for mask in range(group):
        q_got.append(swap(piece(queries, member ^ mask, share, 1), mask))
    for mask in range(group):
        other = member ^ mask
        kv_all = put(kv_all, kv_got[mask], group + other, 0)
        kv_all = put(kv_all, next_level(kv_got[mask]), other, 0)
        marks_all = put(marks_all, marks_got[mask], group + other, 1)
        q_all = put(q_all, q_got[mask], other, 0)
    marks_all = put(marks_all, next_level(marks_all[:, span:]), 0, 1)
    docs_all = marks_all[heads_here]
    docs_all = jnp.where((level == 0) & (jnp.arange(2 * span) < span), -1.0, docs_all)
    aux = jnp.concatenate([piece(marks_all[:heads_here], member, heads, 0), docs_all[None]], axis=0)

    hidden_here = gate_weight.shape[1]
    half = hidden_here // 2
    parity = level % 2

    def from_levels(weight, axis):
        kept = piece(weight, parity, half, axis)
        given = piece(weight, 1 - parity, half, axis)
        shape = list(kept.shape)
        shape[1 - axis] *= levels
        whole = put(jnp.zeros(shape, weight.dtype), kept, level, 1 - axis)
        for steps in range(1, levels):
            got = around(given if steps % 2 else kept, steps)
            whole = put(whole, got, (level - steps) % levels, 1 - axis)
        return whole

    def from_members(weight, axis):
        cut = weight.shape[axis] // 2
        along_x, along_y = swap(weight, 1), swap(weight, 2)
        near = swap(lax.slice_in_dim(along_y, 0, cut, axis=axis), 1)
        far = swap(lax.slice_in_dim(along_x, cut, 2 * cut, axis=axis), 2)
        return [(0, 0, weight), (1, 0, along_x), (2, 0, along_y), (3, 0, near), (3, 1, far)]

    gates = from_members(from_levels(gate_weight, 1), 0)
    ups = from_members(from_levels(up_weight, 1), 0)
    downs = from_members(from_levels(down_weight, 0), 1)

    attended = attend(q_all, kv_all, aux, docs_all, heads, head_size ** (-0.5))

    joined = jnp.zeros((rows, width), jnp.bfloat16)
    for mask in range(group):
        other = member ^ mask
        joined = put(joined, swap(piece(attended, other, rows, 0), mask), other, 1)
    partial_value = jnp.dot(joined, out_weight, preferred_element_type=jnp.float32)
    partial_value = partial_value.astype(jnp.bfloat16)
    own = rows // n_tp
    projected = piece(partial_value, tp_index, own, 0).astype(jnp.float32)
    for steps in range(1, n_tp):
        projected = projected + turn(
            piece(partial_value, (tp_index + steps) % n_tp, own, 0), steps
        ).astype(jnp.float32)
    middle = (piece(residual, tp_index, own, 0).astype(jnp.float32) + projected).astype(
        jnp.bfloat16
    )
    normed = normalize(middle, mix_gain)

    paired = swap(normed, group)
    shared = [turn(part, steps) if steps else part for part in (normed, paired) for steps in range(n_tp)]
    mixer_in = jnp.concatenate(shared, axis=0)
    count, features = mixer_in.shape
    depth = gate_weight.shape[0]
    by_source = mixer_in.reshape(count, levels, group, depth)

    def project(parts):
        total = None
        for mask, order, weight in parts:
            columns = lax.dynamic_slice_in_dim(by_source, member ^ mask, 1, 2).reshape(count, -1)
            columns = piece(columns, order, weight.shape[0], 1)
            term = jnp.dot(columns, weight, preferred_element_type=jnp.float32)
            total = term if total is None else total + term
        return total

    gate_proj, up_proj = project(gates), project(ups)
    hidden = (jax.nn.silu(gate_proj) * up_proj).astype(jnp.bfloat16)

    result = jnp.zeros((own, levels, group, depth), jnp.bfloat16)
    middle_by = middle.reshape(own, levels, group, depth)
    for mask, order, weight in downs:
        lowered = jnp.dot(hidden, weight, preferred_element_type=jnp.float32)
        lowered = lowered.reshape(2, n_tp, own, -1)
        total = lowered[:, 0]
        for steps in range(1, n_tp):
            total = total + turn(lowered[:, steps].astype(jnp.bfloat16), -steps).astype(jnp.float32)
        total = total[0] + swap(total[1].astype(jnp.bfloat16), group).astype(jnp.float32)
        tall = weight.shape[1] // depth
        at = (0, order * tall, member ^ mask, 0)
        part = lax.dynamic_slice(middle_by, at, (own, tall, 1, depth)).astype(jnp.float32)
        part = (part + total.reshape(own, tall, 1, depth)).astype(jnp.bfloat16)
        result = lax.dynamic_update_slice(result, part, at)
    return result.reshape(own, features)


def solution(mesh):
    return jax.shard_map(
        local,
        mesh=mesh,
        in_specs=(
            P("sp", None),
            P("sp", "tp"),
            P("sp", "tp"),
            P("sp", "tp"),
            P("sp", "tp"),
            P("sp"),
            P("tp", None),
            P(),
            P("sp", "tp"),
            P("sp", "tp"),
            P("tp", "sp"),
        ),
        out_specs=P(("sp", "tp"), None),
        check_vma=False,
    )
```

```python
import functools

import jax
import jax.numpy as jnp
from jax import lax
from jax.experimental import pallas as pl
from jax.experimental.pallas import tpu as pltpu
from jax.sharding import PartitionSpec as P

REACH = 4

EPSILON = 1e-06
NEGATIVE = -1e30
LANES = 128


WHOLE = pl.BlockSpec(memory_space=pltpu.VMEM)


def attend_kernel(where_ref, *refs, group, heads, scale):
    qs, kvs, olds, auxes = (refs[i * group : (i + 1) * group] for i in range(4))
    outs = refs[4 * group : 5 * group]
    q_ref, kv_ref, aux_ref, acc_ref = refs[5 * group :]
    rows, width = q_ref.shape
    head_size = width // heads
    member = where_ref[0]
    step = pl.program_id(0)

    @pl.when(step == 0)
    def _():
        for mask in range(group):
            other = member ^ mask
            kv_ref[other] = olds[mask][...]
            kv_ref[group + other] = kvs[mask][...]
            aux = auxes[mask]
            aux_ref[other] = aux[0]
            aux_ref[group + other] = aux[1]

    for mask in range(group):

        @pl.when(step == member ^ mask)
        def _(mask=mask):
            q_ref[...] = qs[mask][...] * jnp.asarray(scale, q_ref.dtype)

    lane = lax.broadcasted_iota(jnp.int32, (1, width), 1) // head_size
    q = q_ref[...]
    q_parts = [jnp.where(lane == h, q, jnp.zeros_like(q)) for h in range(heads)]
    last = aux_ref.shape[1] - 1
    diagonal = group + step
    own_docs = aux_ref[diagonal, last : last + 1, :]
    first_doc = jnp.min(own_docs)
    qdoc = jnp.transpose(jnp.broadcast_to(own_docs, (128, rows)))[:, :1]
    low = step
    for back in range(group):
        before = jnp.max(aux_ref[step + back, last : last + 1, :]) < first_doc
        low = low + before.astype(jnp.int32)
    acc_ref[...] = jnp.zeros_like(acc_ref)

    def chunk(index, carry, causal):
        k = kv_ref[index, :, :width]
        v = kv_ref[index, :, width:]
        seen = aux_ref[index, last : last + 1, :] == qdoc
        if causal:
            row = lax.broadcasted_iota(jnp.int32, (rows, rows), 0)
            col = lax.broadcasted_iota(jnp.int32, (rows, rows), 1)
            seen = seen & (col <= row)
        new = []
        decay = jnp.zeros((rows, width), jnp.float32)
        added = jnp.zeros((rows, width), jnp.float32)
        for h in range(heads):
            top, total = carry[h]
            gate = aux_ref[index, pl.ds(member * heads + h, 1), :]
            scores = lax.dot_general(
                q_parts[h], k, (((1,), (1,)), ((), ())), preferred_element_type=jnp.float32
            )
            scores = jnp.where(seen, scores - gate, NEGATIVE)
            new_top = jnp.maximum(top, jnp.max(scores, axis=-1, keepdims=True))
            weights = jnp.exp(scores - new_top)
            shrink = jnp.exp(top - new_top)
            total = total * shrink + jnp.sum(weights, axis=-1, keepdims=True)
            v_part = jnp.where(lane == h, v, jnp.zeros_like(v))
            added = added + jnp.dot(
                weights.astype(v.dtype), v_part, preferred_element_type=jnp.float32
            )
            decay = jnp.where(lane == h, shrink, decay)
            new.append((new_top, total))
        acc_ref[...] = acc_ref[...] * decay + added
        return tuple(new)

    first = tuple(
        (jnp.full((rows, 1), NEGATIVE, jnp.float32), jnp.zeros((rows, 1), jnp.float32))
        for _ in range(heads)
    )
    carry = lax.fori_loop(low, diagonal, functools.partial(chunk, causal=False), first)
    carry = chunk(diagonal, carry, True)
    divisor = jnp.ones((rows, width), jnp.float32)
    for h in range(heads):
        divisor = jnp.where(lane == h, carry[h][1], divisor)
    value = (acc_ref[...] / divisor).astype(jnp.bfloat16)
    for mask in range(group):

        @pl.when(step == member ^ mask)
        def _(mask=mask):
            outs[mask][...] = value


def attend(member, qs, kvs, olds, auxes, heads, scale):
    group = len(qs)
    rows, width = qs[0].shape
    aux_shape = (2 * group,) + auxes[0].shape[1:]
    span = group * rows
    return pl.pallas_call(
        functools.partial(attend_kernel, group=group, heads=heads, scale=scale),
        grid=(group,),
        in_specs=[pl.BlockSpec(memory_space=pltpu.SMEM)] + [WHOLE] * (4 * group),
        out_specs=[WHOLE] * group,
        scratch_shapes=[
            pltpu.VMEM((rows, width), jnp.bfloat16),
            pltpu.VMEM((2 * group, rows, 2 * width), jnp.bfloat16),
            pltpu.VMEM(aux_shape, jnp.float32),
            pltpu.VMEM((rows, width), jnp.float32),
        ],
        out_shape=[jax.ShapeDtypeStruct((rows, width), jnp.bfloat16)] * group,
        cost_estimate=pl.CostEstimate(
            flops=4 * span * span * width * heads,
            bytes_accessed=8 * span * width * 2,
            transcendentals=span * span * heads,
        ),
        name="attend",
    )(member[None], *qs, *kvs, *olds, *auxes)


def project_kernel(where_ref, *refs, group, parts):
    member, place = where_ref[0], where_ref[1]
    pieces, weight_ref, outs = refs[:group], refs[group], refs[group + 1 :]
    rows, width = pieces[0].shape
    own = rows // parts
    for part in range(parts):
        start = pl.multiple_of(lax.rem(place + part, parts) * own, own)
        total = None
        for mask in range(group):
            at = pl.multiple_of((member ^ mask) * width, width)
            term = jnp.dot(
                pieces[mask][pl.ds(start, own), :],
                weight_ref[pl.ds(at, width), :],
                preferred_element_type=jnp.float32,
            )
            total = term if total is None else total + term
        outs[part][...] = total.astype(jnp.bfloat16)


def project(member, place, pieces, weight, parts):
    group = len(pieces)
    rows, width = pieces[0].shape
    features = weight.shape[1]
    block = features // 4
    own = rows // parts
    return pl.pallas_call(
        functools.partial(project_kernel, group=group, parts=parts),
        grid=(4,),
        in_specs=[pl.BlockSpec(memory_space=pltpu.SMEM)]
        + [WHOLE] * group
        + [pl.BlockSpec((weight.shape[0], block), lambda i: (0, i))],
        out_specs=[pl.BlockSpec((own, block), lambda i: (0, i))] * parts,
        out_shape=[jax.ShapeDtypeStruct((own, features), jnp.bfloat16)] * parts,
        cost_estimate=pl.CostEstimate(
            flops=2 * rows * width * group * features,
            bytes_accessed=2 * weight.size,
            transcendentals=0,
        ),
        name="project",
    )(jnp.stack([member, place]), *pieces, weight)


def middle_kernel(where_ref, residual_ref, *refs, parts, levels, group):
    device, place = where_ref[0], where_ref[1]
    partials, gain_ref = refs[:parts], refs[parts]
    middle_ref, mine_ref, theirs_ref, normed_ref = refs[parts + 1 :]
    own = middle_ref.shape[0]
    total = partials[0][...].astype(jnp.float32)
    for part in partials[1:]:
        total = total + part[...].astype(jnp.float32)
    start = pl.multiple_of(place * own, own)
    middle = (residual_ref[pl.ds(start, own), :].astype(jnp.float32) + total).astype(jnp.bfloat16)
    middle_ref[...] = middle
    widened = middle.astype(jnp.float32)
    factor = lax.rsqrt(jnp.mean(widened * widened, axis=-1, keepdims=True) + EPSILON)
    normed_ref[...] = (widened * factor * gain_ref[...]).astype(jnp.bfloat16)
    depth = middle_ref.shape[1] // (levels * group)
    if depth % LANES:
        mine_ref[...] = normed_ref[...]
        theirs_ref[...] = normed_ref[...]
        return
    for mask in range(group):
        for level in range(levels):
            source = device ^ (level * group + mask)
            block = normed_ref[:, pl.ds(pl.multiple_of(source * depth, depth), depth)]
            at = (mask * levels + level) * depth
            mine_ref[:, at : at + depth] = block
            at = (mask * levels + (level ^ 1)) * depth
            theirs_ref[:, at : at + depth] = block


def make_middle(device, place, residual, partials, gain, levels, group):
    own, features = partials[0].shape
    shape = jax.ShapeDtypeStruct((own, features), jnp.bfloat16)
    middle, mine, theirs = pl.pallas_call(
        functools.partial(middle_kernel, parts=len(partials), levels=levels, group=group),
        in_specs=[pl.BlockSpec(memory_space=pltpu.SMEM)] + [WHOLE] * (len(partials) + 2),
        out_specs=[WHOLE] * 3,
        out_shape=[shape] * 3,
        scratch_shapes=[pltpu.VMEM((own, features), jnp.bfloat16)],
        cost_estimate=pl.CostEstimate(
            flops=2000 * own * features, bytes_accessed=10 * own * features, transcendentals=own
        ),
        name="middle",
    )(jnp.stack([device, place]), residual, *partials, gain[None])
    depth = features // (levels * group)
    if depth % LANES:
        order = jnp.arange(levels * group, dtype=jnp.int32)
        mask, kept = order // levels, order % levels
        blocks = mine.reshape(own, levels * group, depth)
        mine = jnp.take(blocks, device ^ (kept * group + mask), axis=1).reshape(own, features)
        theirs = jnp.take(blocks, device ^ ((kept ^ 1) * group + mask), axis=1)
        theirs = theirs.reshape(own, features)
    return middle, mine, theirs


def mix_kernel(*refs, blocks, offsets):
    count = len(offsets)
    xs, gates, ups = refs[:blocks], refs[blocks : blocks + count], refs[blocks + count : blocks + 2 * count]
    out_ref, x_ref = refs[blocks + 2 * count :]
    own = xs[0].shape[0]

    @pl.when(pl.program_id(0) == 0)
    def _():
        for index in range(blocks):
            x_ref[index * own : (index + 1) * own, :] = xs[index][...]

    def product(parts):
        total = None
        for offset, part in zip(offsets, parts):
            term = jnp.dot(
                x_ref[:, offset : offset + part.shape[0]],
                part[...],
                preferred_element_type=jnp.float32,
            )
            total = term if total is None else total + term
        return total

    gate, up = product(gates), product(ups)
    out_ref[...] = (gate / (1.0 + jnp.exp(-gate)) * up).astype(jnp.bfloat16)


def mix(xs, gates, ups):
    own, features = xs[0].shape
    rows = own * len(xs)
    hidden = gates[0].shape[1]
    block = next(size for size in (256, 128, hidden) if hidden % size == 0)
    offsets, at = [], 0
    for part in gates:
        offsets.append(at)
        at += part.shape[0]
    weights = [pl.BlockSpec((part.shape[0], block), lambda i: (0, i)) for part in gates]
    return pl.pallas_call(
        functools.partial(mix_kernel, blocks=len(xs), offsets=tuple(offsets)),
        grid=(hidden // block,),
        in_specs=[WHOLE] * len(xs) + weights + weights,
        out_specs=pl.BlockSpec((rows, block), lambda i: (0, i)),
        out_shape=jax.ShapeDtypeStruct((rows, hidden), jnp.bfloat16),
        scratch_shapes=[pltpu.VMEM((rows, features), jnp.bfloat16)],
        cost_estimate=pl.CostEstimate(
            flops=4 * rows * features * hidden,
            bytes_accessed=4 * features * hidden + 2 * rows * (features + hidden),
            transcendentals=rows * hidden,
        ),
        name="mix",
    )(*xs, *gates, *ups)


def final_kernel(where_ref, middle_ref, *refs, levels, group, shapes):
    device = where_ref[0]
    kept, got, out_ref = refs[: len(shapes)], refs[len(shapes) : 2 * len(shapes)], refs[-1]
    depth = middle_ref.shape[1] // (levels * group)
    for index, (mask, first) in enumerate(shapes):
        for column in range(kept[index].shape[1] // depth):
            level = first + column
            at = pl.ds(pl.multiple_of((device ^ (level * group + mask)) * depth, depth), depth)
            mine = slice(column * depth, (column + 1) * depth)
            theirs = slice((column ^ 1) * depth, ((column ^ 1) + 1) * depth)
            total = kept[index][:, mine] + got[index][:, theirs].astype(jnp.float32)
            out_ref[:, at] = (middle_ref[:, at].astype(jnp.float32) + total).astype(out_ref.dtype)


def finish(device, middle, kept, got, shapes, levels, group):
    own, features = middle.shape
    depth = features // (levels * group)
    if depth % LANES:
        place = device ^ jnp.arange(levels * group, dtype=jnp.int32)
        mask, column = place % group, place // group
        kept = jnp.concatenate(kept, axis=1).reshape(own, -1, depth)
        got = jnp.concatenate(got, axis=1).reshape(own, -1, depth).astype(jnp.float32)
        total = jnp.take(kept, mask * levels + column, axis=1)
        total = total + jnp.take(got, mask * levels + (column ^ 1), axis=1)
        return (middle.astype(jnp.float32) + total.reshape(own, features)).astype(middle.dtype)
    return pl.pallas_call(
        functools.partial(final_kernel, levels=levels, group=group, shapes=tuple(shapes)),
        in_specs=[pl.BlockSpec(memory_space=pltpu.SMEM)] + [WHOLE] * (1 + 2 * len(shapes)),
        out_specs=WHOLE,
        out_shape=jax.ShapeDtypeStruct(middle.shape, middle.dtype),
        cost_estimate=pl.CostEstimate(
            flops=2000 * middle.size, bytes_accessed=10 * middle.size, transcendentals=0
        ),
        name="finish",
    )(device[None], middle, *kept, *got)


def local(
    residual,
    queries,
    keys,
    values,
    gate_cache,
    doc_ids,
    out_weight,
    mix_gain,
    gate_weight,
    up_weight,
    down_weight,
):
    n_sp, n_tp = lax.axis_size("sp"), lax.axis_size("tp")
    group = REACH
    levels = n_sp // group
    sp_index, tp_index = lax.axis_index("sp"), lax.axis_index("tp")
    level, member = sp_index // group, sp_index % group
    rows, width = queries.shape
    heads_here = gate_cache.shape[1]
    head_size = width // heads_here
    heads = heads_here // group
    share = width // group
    own = rows // n_tp

    def swap(value, mask):
        return lax.ppermute(value, "sp", [(s, s ^ mask) for s in range(n_sp)])

    def next_level(value):
        return lax.ppermute(value, "sp", [(s, s + group) for s in range(n_sp - group)])

    def turn(value, steps):
        return lax.ppermute(value, "tp", [(t, (t + steps) % n_tp) for t in range(n_tp)])

    def piece(value, index, size, axis):
        return lax.dynamic_slice_in_dim(value, index * size, size, axis)

    def cut_kv(other):
        return jnp.concatenate(
            [piece(keys, other, share, 1), piece(values, other, share, 1)], axis=1
        )

    others = range(1, group)
    kvs = [cut_kv(member)] + [swap(cut_kv(member ^ m), m) for m in others]
    olds = [next_level(kvs[m]) for m in range(group)]
    qs = [piece(queries, member, share, 1)]
    qs += [swap(piece(queries, member ^ m, share, 1), m) for m in others]
    marks = jnp.concatenate([gate_cache.T, doc_ids.astype(jnp.float32)[None] + 1.0], axis=0)
    marks = jnp.stack([next_level(marks), marks])
    auxes = [marks] + [swap(marks, m) for m in others]

    half = gate_weight.shape[1] // 2
    parity = level % 2

    def from_levels(weight, axis):
        kept = piece(weight, parity, half, axis)
        given = piece(weight, 1 - parity, half, axis)
        parts = [kept]
        for distance in range(1, levels):
            parts.append(swap(given if distance % 2 else kept, distance * group))
        return jnp.concatenate(parts, axis=1 - axis)

    def from_members(weight, axis):
        middle = weight.shape[axis] // 2
        along_x, along_y = swap(weight, 1), swap(weight, 2)
        near = swap(lax.slice_in_dim(along_y, 0, middle, axis=axis), 1)
        far = swap(lax.slice_in_dim(along_x, middle, 2 * middle, axis=axis), 2)
        return [weight, along_x, along_y, near, far]

    gates = from_members(from_levels(gate_weight, 1), 0)
    ups = from_members(from_levels(up_weight, 1), 0)
    downs = from_members(from_levels(down_weight, 0), 1)

    attended = attend(member, qs, kvs, olds, auxes, heads, head_size ** (-0.5))

    pieces = [attended[0]] + [swap(attended[m], m) for m in others]
    partials = project(member, tp_index, pieces, out_weight, n_tp)
    partials = [partials[0]] + [turn(partials[steps], steps) for steps in range(1, n_tp)]
    middle, mine, theirs = make_middle(
        sp_index, tp_index, residual, partials, mix_gain, levels, group
    )

    theirs = swap(theirs, group)
    xs = [mine] + [turn(mine, steps) for steps in range(1, n_tp)]
    xs += [theirs] + [turn(theirs, steps) for steps in range(1, n_tp)]
    hidden = mix(xs, gates, ups)

    kept, got, shapes = [], [], []
    for index, (mask, first) in enumerate(((0, 0), (1, 0), (2, 0), (3, 0), (3, levels // 2))):
        lowered = jnp.dot(hidden, downs[index], preferred_element_type=jnp.float32)
        lowered = lowered.reshape(2, n_tp, own, -1)
        total = lowered[:, 0]
        for steps in range(1, n_tp):
            sent = lowered[:, steps].astype(jnp.bfloat16)
            total = total + turn(sent, -steps).astype(jnp.float32)
        kept.append(total[0])
        got.append(swap(total[1].astype(jnp.bfloat16), group))
        shapes.append((mask, first))
    return finish(sp_index, middle, kept, got, shapes, levels, group)


def solution(mesh):
    return jax.shard_map(
        local,
        mesh=mesh,
        in_specs=(
            P("sp", None),
            P("sp", "tp"),
            P("sp", "tp"),
            P("sp", "tp"),
            P("sp", "tp"),
            P("sp"),
            P("tp", None),
            P(),
            P("sp", "tp"),
            P("sp", "tp"),
            P("tp", "sp"),
        ),
        out_specs=P(("sp", "tp"), None),
        check_vma=False,
    )
```
